32 devices in a mesh: ep: 8 (over z, x), tp: 4 (over y, core).
Axes of the slice: x: 2, y: 2, z: 4, core: 2. Of those that a mesh axis runs over, the one named last changes fastest.
Arguments:
- tokens: bfloat16 [8192, 2048], P(('ep', 'tp')), may hold values from -6 to 6
- pre_gain: float32 [2048], replicated, may hold values from 0.1 to 1.9
- post_gain: float32 [2048], replicated, may hold values from 0.1 to 1.9
- expert_ids: int32 [8192, 2], P(('ep', 'tp')), may hold values from 0 to 7, as said below
- route_weight: float32 [8192, 2], P(('ep', 'tp')), may hold values from 0.1 to 1
- w_gate: bfloat16 [8, 2048, 512], P('ep', None, 'tp'), may hold values from -0.125 to 0.125
- w_up: bfloat16 [8, 2048, 512], P('ep', None, 'tp'), may hold values from -0.125 to 0.125
- w_down: bfloat16 [8, 2048, 512], P('ep', None, 'tp'), may hold values from -0.25 to 0.25
Outputs:
- layer_out: bfloat16 [8192, 2048], P(('ep', 'tp'))
The draws below stay inside these ranges and needn't reach their ends.
Inputs may be any that keep to these rules, and one draw needn't show every extreme that they name: `expert_ids`: each token names two different experts of one group, group g being experts 4 * g to 4 * g + 3. Among the rows of one device (aligned blocks of 256 rows) no expert is named more than 128 times, and in every block some expert is named exactly 128 times; one expert is named 128 times in every block.
All inputs are finite; a program needn't handle non-finite values.
Results may differ from the reference program's by a relative error of at most 0.0071.
Values may be sent and summed in bfloat16 or wider, within the bound.
No kernel may reach another device: no remote copies, remote signals or barrier semaphores. Data moves between devices by JAX's collectives and lax.ppermute only.
A program may use at most 64 MiB of HBM per device.

```python
import math
import jax
import jax.numpy as jnp
from jax import lax

D = 2048
FF = 512
TOP = 2
GROUP = 4
TOK_DEV = 256
EXPERTS = 8
CAP = 128
TOKENS = 8192


def draw_expert_ids(key, part):
    blocks = TOKENS // TOK_DEV
    share = TOP * TOK_DEV // EXPERTS
    pairs = EXPERTS // (2 * GROUP)
    star = jax.random.randint(jax.random.fold_in(key, 11), (), 0, EXPERTS)
    star_group = star // GROUP
    star_pair = star_group // 2
    star_side = star_group % 2
    star_local = star % GROUP
    place = jnp.arange(2 * share * 2, dtype=jnp.int32)
    hot_three = 3 * share
    first_role = jnp.where(place < 2 * share, 0, jnp.where(place < hot_three, 1, jnp.where(place < hot_three + share // 2, 0, 2)))
    second_role = jnp.where(place < share, 1, jnp.where(place < 2 * share, 2, jnp.where(place < hot_three, 3, jnp.where(place < hot_three + share // 2, 1, 3))))
    is_hot = place < hot_three

    def one_block(block):
        block_key = jax.random.fold_in(key, block)
        hot_side = jax.random.randint(jax.random.fold_in(block_key, 1), (pairs,), 0, 2)
        hot_side = jnp.where(jnp.arange(pairs) == star_pair, star_side, hot_side)
        perm_keys = jax.random.split(jax.random.fold_in(block_key, 2), 2 * pairs)
        perms = jax.vmap(lambda sub: jax.random.permutation(sub, GROUP))(perm_keys).astype(jnp.int32)
        star_row = perms[star_group]
        where_star = jnp.argmax(star_row == star_local)
        star_row = star_row.at[where_star].set(star_row[0]).at[0].set(star_local)
        perms = perms.at[star_group].set(star_row)
        pair_index = jnp.arange(pairs, dtype=jnp.int32)[:, None]
        group = 2 * pair_index + jnp.where(is_hot[None, :], hot_side[:, None], 1 - hot_side[:, None])
        first = group * GROUP + perms[group, first_role[None, :]]
        second = group * GROUP + perms[group, second_role[None, :]]
        both = jnp.stack([first.reshape(-1), second.reshape(-1)], axis=1)
        shuffle = jax.random.permutation(jax.random.fold_in(block_key, 3), TOK_DEV)
        return both[shuffle]
    table = lax.map(one_block, jnp.arange(blocks, dtype=jnp.int32))
    return table.reshape(TOKENS, TOP).astype(jnp.int32)


def block_scale(rng, shape, shards, least, high):
    def one(dim, blocks):
        draws = jax.random.uniform(jax.random.fold_in(jax.random.fold_in(rng, 6), dim), (blocks,), jnp.float32, least / len(shards), high / len(shards))
        return jnp.repeat(jnp.exp(draws), shape[dim] // blocks).reshape((-1,) + (1,) * (len(shape) - dim - 1))

    level = one(*shards[0])
    for cut in shards[1:]:
        level = level * one(*cut)
    return level


def bell_draw(key, shape, spread, reach, cuts=(), kind=jnp.bfloat16):
    array = spread * jax.random.normal(key, shape, jnp.float32)
    if cuts:
        array = array * block_scale(key, shape, cuts, -0.22, 0.18)
    return jnp.clip(array, -reach, reach).astype(kind)


def setup_inputs(seed: int = 0) -> dict:
    streams_of = jax.random.split(jax.random.key(seed), 9)
    tokens = bell_draw(streams_of[0], (TOKENS, D), 1.0, 6.0, ((0, 32),))
    pre_gain = jnp.clip(1.0 + 0.18 * jax.random.normal(streams_of[1], (D,), jnp.float32), 0.1, 1.9)
    post_gain = jnp.clip(1.0 + 0.18 * jax.random.normal(streams_of[2], (D,), jnp.float32), 0.1, 1.9)
    expert_ids = draw_expert_ids(jax.random.fold_in(streams_of[8], 71), 0)
    route_weight = jnp.clip(jnp.exp(math.log(1.0) - 2.3025851 * jax.random.uniform(streams_of[4], (TOKENS, TOP), jnp.float32) ** block_scale(streams_of[4], (TOKENS, TOP), ((0, 32),), -0.2, 0.2)), 0.1, 1.0)
    w_gate = bell_draw(streams_of[5], (EXPERTS, D, FF), D ** -0.5, 0.125, ((0, 8), (2, 4)))
    w_up = bell_draw(streams_of[6], (EXPERTS, D, FF), D ** -0.5, 0.125, ((0, 8), (2, 4)))
    w_down = bell_draw(streams_of[7], (EXPERTS, D, FF), FF ** -0.5, 0.25, ((0, 8), (2, 4)))
    return dict(tokens=tokens, pre_gain=pre_gain, post_gain=post_gain, expert_ids=expert_ids, route_weight=route_weight, w_gate=w_gate, w_up=w_up, w_down=w_down)


def rms_scale(values, gain):
    mean_sq = lax.optimization_barrier(jnp.mean(values * values, axis=-1, keepdims=True))
    return values * lax.rsqrt(mean_sq + 1e-06) * gain

def reference(tokens, pre_gain, post_gain, expert_ids, route_weight, w_gate, w_up, w_down):
    count = tokens.shape[0]
    width = tokens.shape[1]
    normed = rms_scale(tokens.astype(jnp.float32), pre_gain).astype(jnp.bfloat16)
    padded = jnp.concatenate([normed, jnp.zeros((1, width), jnp.bfloat16)], axis=0)
    flat = expert_ids.reshape(-1).astype(jnp.int32)
    routes = flat.shape[0]
    order = jnp.argsort(flat, stable=True).astype(jnp.int32)
    sorted_ids = flat[order]
    first = jnp.searchsorted(sorted_ids, sorted_ids, side='left').astype(jnp.int32)
    rank = jnp.arange(routes, dtype=jnp.int32) - first
    global_cap = count // TOK_DEV * CAP
    table = jnp.full((EXPERTS * global_cap,), routes, jnp.int32)
    table = table.at[sorted_ids * global_cap + rank].set(order).reshape(EXPERTS, global_cap)

    def one_expert(index):
        slots = table[index]
        rows = padded[jnp.minimum(slots // TOP, count).astype(jnp.int32)]
        rows = jnp.where((slots < routes)[:, None], rows, jnp.zeros_like(rows))
        gate = jnp.dot(rows, w_gate[index], preferred_element_type=jnp.float32)
        up = jnp.dot(rows, w_up[index], preferred_element_type=jnp.float32)
        hidden = (jax.nn.silu(gate) * up).astype(jnp.bfloat16)
        return jnp.dot(hidden, w_down[index].T, preferred_element_type=jnp.float32).astype(jnp.bfloat16)
    results = lax.map(one_expert, jnp.arange(EXPERTS, dtype=jnp.int32))
    per_route = jnp.zeros((routes + 1, width), jnp.bfloat16)
    per_route = per_route.at[table.reshape(-1)].set(results.reshape(-1, width))
    per_route = per_route[:routes].reshape(count, TOP, width)
    mixed = lax.optimization_barrier(jnp.sum(per_route.astype(jnp.float32) * route_weight[:, :, None], axis=1))
    return rms_scale(mixed, post_gain).astype(jnp.bfloat16)
```

```python
import functools

import jax
import jax.numpy as jnp
from jax import lax
from jax.experimental import pallas as pl
from jax.experimental.pallas import tpu as pltpu
from jax.sharding import PartitionSpec as P

GROUP = 4
EPS = 1e-06


def rms_scale(values, gain):
    mean_sq = jnp.mean(values * values, axis=-1, keepdims=True)
    return values * lax.rsqrt(mean_sq + EPS) * gain


def expert_terms(rows, gate_part, up_part, down_part):
    gate = jnp.dot(rows, gate_part, preferred_element_type=jnp.float32)
    up = jnp.dot(rows, up_part, preferred_element_type=jnp.float32)
    hidden = (jax.nn.silu(gate) * up).astype(jnp.bfloat16)
    return lax.dot_general(
        hidden, down_part, (((1,), (1,)), ((), ())), preferred_element_type=jnp.float32
    )


def collect_expert(w_gate, w_up, w_down):
    return (
        lax.all_gather(w_gate, "tp", axis=2, tiled=True),
        lax.all_gather(w_up, "tp", axis=2, tiled=True),
        lax.all_gather(w_down, "tp", axis=2, tiled=True),
    )


def routed_body(tokens, pre_gain, post_gain, expert_ids, route_weight, w_gate, w_up, w_down):
    count, width = tokens.shape
    top = expert_ids.shape[1]
    experts = lax.axis_size("ep") * w_gate.shape[0]
    capacity = 2 * top * count // experts
    normed = rms_scale(tokens.astype(jnp.float32), pre_gain).astype(jnp.bfloat16)
    flat = expert_ids.reshape(-1)
    onehot = (flat[:, None] == jnp.arange(experts, dtype=jnp.int32)[None, :]).astype(jnp.int32)
    rank = jnp.sum((jnp.cumsum(onehot, axis=0) - onehot) * onehot, axis=1)
    target = flat * capacity + rank
    source = jnp.full((experts * capacity,), count, jnp.int32)
    source = source.at[target].set(jnp.arange(count * top, dtype=jnp.int32) // top)
    padded = jnp.concatenate([normed, jnp.zeros((1, width), jnp.bfloat16)], axis=0)
    outgoing = padded[source].reshape(experts, capacity, width)
    arrived = lax.all_to_all(outgoing, "ep", split_axis=0, concat_axis=0, tiled=True)
    rows = arrived.reshape(experts * capacity, width)
    gate_all, up_all, down_all = collect_expert(w_gate, w_up, w_down)
    result = expert_terms(rows, gate_all[0], up_all[0], down_all[0])
    answer = result.astype(jnp.bfloat16).reshape(experts, capacity, width)
    returned = lax.all_to_all(answer, "ep", split_axis=0, concat_axis=0, tiled=True)
    per_route = returned.reshape(experts * capacity, width)[target].reshape(count, top, width)
    mixed = jnp.sum(per_route.astype(jnp.float32) * route_weight[:, :, None], axis=1)
    return rms_scale(mixed, post_gain).astype(jnp.bfloat16)


def swap(value, axis, bit):
    size = lax.axis_size(axis)
    return lax.ppermute(value, axis, [(i, i ^ bit) for i in range(size)])


def hidden_kernel(first, blocks, *refs):
    mix = refs[:blocks]
    rows = refs[blocks : 2 * blocks]
    g0, g1, u0, u1, out = refs[2 * blocks :]
    count = rows[0].shape[0]
    for b in range(blocks):
        x = rows[b][...]
        scale = jnp.transpose(mix[b][...])[:, 2 * b + first : 2 * b + first + 1]
        for part, (g, u) in enumerate(((g0, u0), (g1, u1))):
            gate = jnp.dot(x, g[...], preferred_element_type=jnp.float32)
            up = jnp.dot(x, u[...], preferred_element_type=jnp.float32)
            value = gate / (1.0 + jnp.exp(-gate)) * up * scale
            width = g.shape[1]
            out[b * count : (b + 1) * count, part * width : (part + 1) * width] = value.astype(out.dtype)


def hidden_call(first, mixes, rows, g, u):
    blocks = len(rows)
    count, width = rows[0].shape
    units = g[0].shape[1]
    flops = 2 * blocks * count * width * 4 * units
    return pl.pallas_call(
        functools.partial(hidden_kernel, first, blocks),
        out_shape=jax.ShapeDtypeStruct((blocks * count, 2 * units), jnp.bfloat16),
        in_specs=[pl.BlockSpec(memory_space=pltpu.VMEM)] * (2 * blocks + 4),
        out_specs=pl.BlockSpec(memory_space=pltpu.VMEM),
        cost_estimate=pl.CostEstimate(flops=flops, bytes_accessed=2 * width * (blocks * count + 4 * units), transcendentals=0),
        name="hidden",
    )(*mixes, *rows, *g, *u)


def down_kernel(starts, *refs):
    hidden = refs[:4]
    pieces = refs[4:12]
    outs = refs[12:]
    count = outs[0].shape[0]
    width = outs[0].shape[1]
    step = min(width, 512)
    for c in range(0, width, step):
        mats = [
            jnp.concatenate([pieces[2 * i][c : c + step, :], pieces[2 * i + 1][c : c + step, :]], axis=1)
            for i in range(4)
        ]
        for out, start in zip(outs, starts):
            total = None
            for i in range(4):
                term = lax.dot_general(
                    hidden[i][start : start + count, :], mats[i],
                    (((1,), (1,)), ((), ())), preferred_element_type=jnp.float32,
                )
                total = term if total is None else total + term
            out[:, c : c + step] = total.astype(out.dtype)


def down_call(starts, count, hidden, pieces):
    width = pieces[0].shape[0]
    units = sum(p.shape[1] for p in pieces)
    flops = 2 * len(starts) * count * width * units
    shape = jax.ShapeDtypeStruct((count, width), jnp.bfloat16)
    return pl.pallas_call(
        functools.partial(down_kernel, starts),
        out_shape=[shape] * len(starts),
        in_specs=[pl.BlockSpec(memory_space=pltpu.VMEM)] * 12,
        out_specs=[pl.BlockSpec(memory_space=pltpu.VMEM)] * len(starts),
        cost_estimate=pl.CostEstimate(flops=flops, bytes_accessed=2 * width * (units + len(starts) * count), transcendentals=0),
        name="down",
    )(*hidden, *pieces)


def paired_body(tokens, pre_gain, post_gain, expert_ids, route_weight, w_gate, w_up, w_down):
    count, width = tokens.shape
    half = count // 2
    me = lax.axis_index("ep")
    row = jnp.arange(2 * GROUP, dtype=jnp.int32)
    named = me ^ (row // 2) ^ ((row % 2) * GROUP)
    mix = jnp.sum(
        jnp.where(expert_ids.T[None, :, :] == named[:, None, None], route_weight.T[None, :, :], 0.0), axis=1
    )
    mix_x = swap(mix, "ep", 1)
    mix_z = swap(mix, "ep", 2)
    mix_d = swap(mix_z, "ep", 1)

    tok_z = swap(tokens, "ep", 2)
    tok_x = swap(tokens, "ep", 1)
    near = [w_gate[0], w_up[0], w_down[0]]
    far = [swap(w, "ep", GROUP) for w in near]
    near_y = [swap(w, "tp", 2) for w in near]
    tok_d = jnp.concatenate([swap(tok_z[:half], "ep", 1), swap(tok_x[half:], "ep", 2)], axis=0)
    far_y = [swap(w, "tp", 2) for w in far]
    near_c = [swap(w, "tp", 1) for w in near]
    near_yc = [swap(w, "tp", 1) for w in near_y]
    far_c = [swap(w, "tp", 1) for w in far]
    far_yc = [swap(w, "tp", 1) for w in far_y]

    blocks = [tokens, tok_x, tok_z, tok_d]
    rows = [rms_scale(b.astype(jnp.float32), pre_gain).astype(jnp.bfloat16) for b in blocks]
    mixes = [mix, mix_x, mix_z, mix_d]
    hidden = []
    for first, a, b in ((0, near, near_c), (0, near_y, near_yc), (1, far, far_c), (1, far_y, far_yc)):
        hidden.append(hidden_call(first, mixes, rows, (a[0], b[0]), (a[1], b[1])))
    pieces = [v[2] for v in (near, near_c, near_y, near_yc, far, far_c, far_y, far_yc)]

    (out_d,) = down_call((3 * count,), count, hidden, pieces)
    got_x = swap(out_d[:half], "ep", 1)
    got_z = swap(out_d[half:], "ep", 2)
    out_x, out_z = down_call((count, 2 * count), count, hidden, pieces)
    (out_own,) = down_call((0,), count, hidden, pieces)

    def add(a, b):
        return (a.astype(jnp.float32) + b.astype(jnp.float32)).astype(jnp.bfloat16)

    send_z = jnp.concatenate([add(out_z[:half], got_x), out_z[half:]], axis=0)
    send_x = jnp.concatenate([out_x[:half], add(out_x[half:], got_z)], axis=0)
    back_z = swap(send_z, "ep", 2)
    back_x = swap(send_x, "ep", 1)
    mixed = out_own.astype(jnp.float32) + back_z.astype(jnp.float32) + back_x.astype(jnp.float32)
    return rms_scale(mixed, post_gain).astype(jnp.bfloat16)


def body(*args):
    paired = lax.axis_size("ep") == 2 * GROUP and lax.axis_size("tp") == 4
    paired = paired and args[-1].shape[0] == 1 and args[0].shape[0] % 16 == 0
    return (paired_body if paired else routed_body)(*args)


def solution(mesh):
    in_specs = (
        P(("ep", "tp"), None),
        P(),
        P(),
        P(("ep", "tp"), None),
        P(("ep", "tp"), None),
        P("ep", None, "tp"),
        P("ep", None, "tp"),
        P("ep", None, "tp"),
    )
    out_specs = P(("ep", "tp"), None)
    return jax.shard_map(body, mesh=mesh, in_specs=in_specs, out_specs=out_specs, check_vma=False)
```

```python
import functools

import jax
import jax.numpy as jnp
from jax import lax
from jax.experimental import pallas as pl
from jax.experimental.pallas import tpu as pltpu
from jax.sharding import PartitionSpec as P

GROUP = 4
EPS = 1e-06
SLICES = 4


def rms_scale(values, gain):
    mean_sq = jnp.mean(values * values, axis=-1, keepdims=True)
    return values * lax.rsqrt(mean_sq + EPS) * gain


def expert_terms(rows, gate_part, up_part, down_part):
    gate = jnp.dot(rows, gate_part, preferred_element_type=jnp.float32)
    up = jnp.dot(rows, up_part, preferred_element_type=jnp.float32)
    hidden = (jax.nn.silu(gate) * up).astype(jnp.bfloat16)
    return lax.dot_general(
        hidden, down_part, (((1,), (1,)), ((), ())), preferred_element_type=jnp.float32
    )


def collect_expert(w_gate, w_up, w_down):
    return (
        lax.all_gather(w_gate, "tp", axis=2, tiled=True),
        lax.all_gather(w_up, "tp", axis=2, tiled=True),
        lax.all_gather(w_down, "tp", axis=2, tiled=True),
    )


def routed_body(tokens, pre_gain, post_gain, expert_ids, route_weight, w_gate, w_up, w_down):
    count, width = tokens.shape
    top = expert_ids.shape[1]
    experts = lax.axis_size("ep") * w_gate.shape[0]
    capacity = 2 * top * count // experts
    normed = rms_scale(tokens.astype(jnp.float32), pre_gain).astype(jnp.bfloat16)
    flat = expert_ids.reshape(-1)
    onehot = (flat[:, None] == jnp.arange(experts, dtype=jnp.int32)[None, :]).astype(jnp.int32)
    rank = jnp.sum((jnp.cumsum(onehot, axis=0) - onehot) * onehot, axis=1)
    target = flat * capacity + rank
    source = jnp.full((experts * capacity,), count, jnp.int32)
    source = source.at[target].set(jnp.arange(count * top, dtype=jnp.int32) // top)
    padded = jnp.concatenate([normed, jnp.zeros((1, width), jnp.bfloat16)], axis=0)
    outgoing = padded[source].reshape(experts, capacity, width)
    arrived = lax.all_to_all(outgoing, "ep", split_axis=0, concat_axis=0, tiled=True)
    rows = arrived.reshape(experts * capacity, width)
    gate_all, up_all, down_all = collect_expert(w_gate, w_up, w_down)
    result = expert_terms(rows, gate_all[0], up_all[0], down_all[0])
    answer = result.astype(jnp.bfloat16).reshape(experts, capacity, width)
    returned = lax.all_to_all(answer, "ep", split_axis=0, concat_axis=0, tiled=True)
    per_route = returned.reshape(experts * capacity, width)[target].reshape(count, top, width)
    mixed = jnp.sum(per_route.astype(jnp.float32) * route_weight[:, :, None], axis=1)
    return rms_scale(mixed, post_gain).astype(jnp.bfloat16)


def swap(value, axis, bit):
    size = lax.axis_size(axis)
    return lax.ppermute(value, axis, [(i, i ^ bit) for i in range(size)])


def tie(value, *deps):
    return lax.optimization_barrier((value, deps))[0]


def vmem(count):
    return [pl.BlockSpec(memory_space=pltpu.VMEM)] * count


def params(mib):
    return pltpu.CompilerParams(vmem_limit_bytes=mib << 20)


def norm_kernel(x_ref, gain_ref, out_ref):
    x = x_ref[...].astype(jnp.float32)
    out_ref[...] = rms_scale(x, gain_ref[...]).astype(out_ref.dtype)


def norm_call(x, gain):
    return pl.pallas_call(
        norm_kernel,
        out_shape=jax.ShapeDtypeStruct(x.shape, jnp.bfloat16),
        in_specs=vmem(2),
        out_specs=vmem(1)[0],
        compiler_params=params(10),
        cost_estimate=pl.CostEstimate(flops=8 * x.size, bytes_accessed=4 * x.size, transcendentals=0),
        name="norm",
    )(x, gain[None, :])


def hidden_kernel(first, blocks, *refs):
    mix = refs[:blocks]
    rows = refs[blocks : 2 * blocks]
    g0, g1, u0, u1, out = refs[2 * blocks :]
    count = rows[0].shape[0]
    g = jnp.concatenate([g0[...], g1[...]], axis=1)
    u = jnp.concatenate([u0[...], u1[...]], axis=1)
    for b in range(blocks):
        x = rows[b][...]
        scale = jnp.transpose(mix[b][...])[:, 2 * b + first : 2 * b + first + 1]
        gate = jnp.dot(x, g, preferred_element_type=jnp.float32)
        up = jnp.dot(x, u, preferred_element_type=jnp.float32)
        value = gate / (1.0 + jnp.exp(-gate)) * up * scale
        out[b * count : (b + 1) * count, :] = value.astype(out.dtype)


def hidden_call(first, mixes, rows, g, u):
    blocks = len(rows)
    count, width = rows[0].shape
    units = g[0].shape[1]
    flops = 2 * blocks * count * width * 4 * units
    return pl.pallas_call(
        functools.partial(hidden_kernel, first, blocks),
        out_shape=jax.ShapeDtypeStruct((blocks * count, 2 * units), jnp.bfloat16),
        in_specs=vmem(2 * blocks + 4),
        out_specs=vmem(1)[0],
        compiler_params=params(20),
        cost_estimate=pl.CostEstimate(flops=flops, bytes_accessed=2 * width * (blocks * count + 4 * units), transcendentals=0),
        name="hidden",
    )(*mixes, *rows, *g, *u)


def down_kernel(*refs):
    hidden = refs[:4]
    pieces = refs[4:12]
    outs = refs[12:]
    mats = [
        jnp.concatenate([pieces[2 * i][...], pieces[2 * i + 1][...]], axis=1) for i in range(4)
    ]
    count = outs[-1].shape[0]
    half = count // 2
    starts = (3 * count, 3 * count + half, count, count + half, 2 * count, 2 * count + half, 0)
    for out, start in zip(outs, starts):
        total = None
        for i in range(4):
            term = lax.dot_general(
                hidden[i][start : start + out.shape[0], :], mats[i],
                (((1,), (1,)), ((), ())), preferred_element_type=jnp.float32,
            )
            total = term if total is None else total + term
        out[...] = total.astype(out.dtype)


def down_call(hidden, pieces):
    width = pieces[0].shape[0]
    units = sum(p.shape[1] for p in pieces)
    rows = hidden[0].shape[0]
    count = rows // 4
    flops = 2 * rows * width * units
    part = jax.ShapeDtypeStruct((count // 2, width), jnp.bfloat16)
    return pl.pallas_call(
        down_kernel,
        out_shape=[part] * 6 + [jax.ShapeDtypeStruct((count, width), jnp.bfloat16)],
        in_specs=vmem(12),
        out_specs=vmem(7),
        compiler_params=params(20),
        cost_estimate=pl.CostEstimate(flops=flops, bytes_accessed=2 * (width + rows) * (units + width), transcendentals=0),
        name="down",
    )(*hidden, *pieces)


def add_kernel(a_ref, b_ref, out_ref):
    total = a_ref[...].astype(jnp.float32) + b_ref[...].astype(jnp.float32)
    out_ref[...] = total.astype(out_ref.dtype)


def add_call(a, b):
    return pl.pallas_call(
        add_kernel,
        out_shape=jax.ShapeDtypeStruct(a.shape, a.dtype),
        in_specs=vmem(2),
        out_specs=vmem(1)[0],
        compiler_params=params(6),
        cost_estimate=pl.CostEstimate(flops=a.size, bytes_accessed=6 * a.size, transcendentals=0),
        name="add",
    )(a, b)


def final_kernel(slices, gain_ref, *refs):
    out = refs[-1]
    count = out.shape[0]
    half = count // 2
    for part in range(2):
        rows = slice(part * half, (part + 1) * half)
        sums = []
        for s in range(slices):
            own, z0, z1, x0, x1 = refs[5 * s : 5 * s + 5]
            total = own[rows, :].astype(jnp.float32)
            total = total + (z0, z1)[part][...].astype(jnp.float32)
            sums.append(total + (x0, x1)[part][...].astype(jnp.float32))
        mixed = jnp.concatenate(sums, axis=1)
        out[rows, :] = rms_scale(mixed, gain_ref[...]).astype(out.dtype)


def final_call(gain, parts):
    count = parts[0][0].shape[0]
    width = sum(p[0].shape[1] for p in parts)
    flat = [ref for p in parts for ref in p]
    return pl.pallas_call(
        functools.partial(final_kernel, len(parts)),
        out_shape=jax.ShapeDtypeStruct((count, width), jnp.bfloat16),
        in_specs=vmem(1 + len(flat)),
        out_specs=vmem(1)[0],
        compiler_params=params(20),
        cost_estimate=pl.CostEstimate(flops=10 * count * width, bytes_accessed=8 * count * width, transcendentals=0),
        name="final",
    )(gain[None, :], *flat)


def paired_body(tokens, pre_gain, post_gain, expert_ids, route_weight, w_gate, w_up, w_down):
    count, width = tokens.shape
    half = count // 2
    cut = width // SLICES
    me = lax.axis_index("ep")
    row = jnp.arange(2 * GROUP, dtype=jnp.int32)
    named = me ^ (row // 2) ^ ((row % 2) * GROUP)
    mix = jnp.sum(
        jnp.where(expert_ids.T[None, :, :] == named[:, None, None], route_weight.T[None, :, :], 0.0), axis=1
    )
    gate, up, down = w_gate[0], w_up[0], w_down[0]

    def over_y(v):
        return swap(v, "tp", 2)

    def over_c(v):
        return swap(v, "tp", 1)

    tok_z = swap(tokens, "ep", 2)
    far_g = swap(gate, "ep", GROUP)
    far_u = swap(up, "ep", GROUP)
    tok_x = swap(tokens, "ep", 1)
    y_g, y_u = over_y(gate), over_y(up)
    c_g, c_u, c_d = over_c(gate), over_c(up), over_c(down)
    y_d = over_y(down)
    mix_z = swap(mix, "ep", 2)
    mix_x = swap(mix, "ep", 1)
    mix_d = swap(mix_z, "ep", 1)
    row_own = norm_call(tokens, pre_gain)

    tok_d0 = swap(tok_z[:half], "ep", 1)
    tok_d1 = swap(tok_x[half:], "ep", 2)
    yc_g, yc_u = over_c(tie(y_g, tok_x, tok_z)), over_c(tie(y_u, tok_x, tok_z))
    row_x, row_z = norm_call(tok_x, pre_gain), norm_call(tok_z, pre_gain)

    far_g = tie(far_g, y_g, y_u, tok_x, tok_z, row_x, row_z)
    far_yg, far_cg = over_y(far_g), over_c(far_g)
    yc_d = over_c(tie(y_d, far_g))

    row_d = norm_call(jnp.concatenate([tie(tok_d0, far_g), tie(tok_d1, far_g)], axis=0), pre_gain)
    rows = [row_own, row_x, row_z, row_d]
    mixes = [mix, mix_x, mix_z, mix_d]
    h_near = hidden_call(0, mixes, rows, (gate, c_g), (up, c_u))
    h_y = hidden_call(0, mixes, rows, (y_g, yc_g), (y_u, yc_u))

    far_u = tie(far_u, h_near, h_y)
    far_yu, far_cu = over_y(far_u), over_c(far_u)
    down_cut = [tie(down[s * cut : (s + 1) * cut], far_u) for s in range(SLICES)]
    far_d = [swap(v, "ep", GROUP) for v in down_cut]
    h_far = hidden_call(1, mixes, rows, (far_g, far_cg), (far_u, far_cu))
    far_ycg = over_c(tie(far_yg, h_far))

    far_yd, far_cd, far_ycd = [None] * SLICES, [None] * SLICES, [None] * SLICES
    last = h_far
    for s in range(SLICES):
        if s == 1:
            far_ycu = over_c(tie(far_yu, last))
            h_fy = hidden_call(1, mixes, rows, (far_yg, far_ycg), (far_yu, far_ycu))
            last = h_fy
        far_d[s] = tie(far_d[s], last)
        far_yd[s], far_cd[s] = over_y(far_d[s]), over_c(far_d[s])
        last = far_d[s]

    parts = []
    for s in range(SLICES):
        far_ycd[s] = over_c(far_yd[s])
        span = slice(s * cut, (s + 1) * cut)
        near = [v[span] for v in (down, c_d, y_d, yc_d)]
        d0, d1, x0, x1, z0, z1, own = down_call(
            (h_near, h_y, h_far, h_fy), near + [far_d[s], far_cd[s], far_yd[s], far_ycd[s]]
        )
        got_x, got_z = swap(d0, "ep", 1), swap(d1, "ep", 2)
        back_x0, back_z1 = swap(x0, "ep", 1), swap(z1, "ep", 2)
        back_z0 = swap(add_call(z0, got_x), "ep", 2)
        back_x1 = swap(add_call(x1, got_z), "ep", 1)
        parts.append((own, back_z0, back_z1, back_x0, back_x1))
    return final_call(post_gain, parts)


def body(*args):
    paired = lax.axis_size("ep") == 2 * GROUP and lax.axis_size("tp") == 4
    paired = paired and args[-1].shape[0] == 1 and args[0].shape[0] % 16 == 0
    return (paired_body if paired else routed_body)(*args)


def solution(mesh):
    in_specs = (
        P(("ep", "tp"), None),
        P(),
        P(),
        P(("ep", "tp"), None),
        P(("ep", "tp"), None),
        P("ep", None, "tp"),
        P("ep", None, "tp"),
        P("ep", None, "tp"),
    )
    out_specs = P(("ep", "tp"), None)
    return jax.shard_map(body, mesh=mesh, in_specs=in_specs, out_specs=out_specs, check_vma=False)
```
